32 devices in a mesh: sp: 16 (over z, y, x), tp: 2 (over core).
Axes of the slice: x: 2, y: 2, z: 4, core: 2. Of those that a mesh axis runs over, the one named last changes fastest.
Arguments:
- tokens: bfloat16 [4096, 2048], P('sp', 'tp'), may hold values from -6 to 6
- norm_gain: float32 [2048], replicated, may hold values from 0.1 to 1.9
- glu_value: bfloat16 [2048, 2048], P('sp', 'tp'), may hold values from -0.125 to 0.125
- glu_gate: bfloat16 [2048, 2048], P('sp', 'tp'), may hold values from -0.125 to 0.125
- conv_taps: float32 [31, 2048], P(None, 'tp'), may hold values from -11 to 11
- ln_gain: float32 [2048], P('tp'), may hold values from 0.1 to 1.9
- ln_bias: float32 [2048], P('tp'), may hold values from -3 to 3
- query_weight: bfloat16 [2048, 2048], P('sp', 'tp'), may hold values from -0.125 to 0.125
- key_weight: bfloat16 [2048, 2048], P('sp', 'tp'), may hold values from -0.125 to 0.125
- value_weight: bfloat16 [2048, 2048], P('sp', 'tp'), may hold values from -0.125 to 0.125
- gate_weight: bfloat16 [2048, 32], replicated, may hold values from -0.125 to 0.125
- gate_bias: float32 [32], replicated, may hold values from -1 to 110
- log_decay_extra: float32 [4096, 16], P('sp'), may hold values from -1.3 to 0
- mem_gain: float32 [2048], P('tp'), may hold values from 0.1 to 1.9
- out_conv: bfloat16 [2048, 2048], P('tp'), may hold values from -0.125 to 0.125
- out_mem: bfloat16 [2048, 2048], P('tp'), may hold values from -0.125 to 0.125
Outputs:
- mixed: bfloat16 [4096, 2048], P(('sp', 'tp'))
The draws below stay inside these ranges and needn't reach their ends.
All inputs are finite; a program needn't handle non-finite values.
Results may differ from the reference program's by a relative error of at most 0.015.
Values may be sent and summed in bfloat16 or wider, within the bound.
A program may use at most 128 MiB of HBM per device.

```python
import math
import jax
import jax.numpy as jnp
from jax import lax

D = 2048
CONV = 2048
MEMORY_HEADS = 8
HEAD = 256
KW = 31
BLOCK = 128
MEM = 2048
SEQUENCE_TOKENS = 4096
N_TP = 2


def draw_conv_taps(key, part):
    base_key, rough_key = jax.random.split(jax.random.fold_in(key, 11))
    base = jnp.clip(jax.random.normal(base_key, (KW, CONV), jnp.float32), -4.0, 4.0)
    rising = 10.0 ** (jnp.arange(CONV, dtype=jnp.float32) / CONV)
    rough = jax.random.uniform(rough_key, (1, CONV), jnp.float32, 0.5, 1.5)
    return base * rising[None, :] * rough * KW ** (-0.5)


def draw_gate_bias(key, part):
    input_key, pick_key, fast_key, slow_key = jax.random.split(jax.random.fold_in(key, 23), 4)
    inputs = jax.random.uniform(input_key, (2, MEMORY_HEADS), jnp.float32, -1.0, 1.0)
    share = 0.5
    fast = jax.random.uniform(pick_key, (2, MEMORY_HEADS), jnp.float32) < share
    fast_bias = jax.random.uniform(fast_key, (2, MEMORY_HEADS), jnp.float32, 3.4, 4.6)
    slow_bias = math.log(SEQUENCE_TOKENS) + 1.0 + jax.random.uniform(slow_key, (2, MEMORY_HEADS), jnp.float32, 0.0, 1.0)
    forget = jnp.where(fast, fast_bias, slow_bias)
    return jnp.stack([inputs[0], forget[0], inputs[1], forget[1]]).reshape(4 * MEMORY_HEADS)


def draw_log_decay_extra(key, part):
    rate_key, place_key, loss_key = jax.random.split(jax.random.fold_in(key, 37), 3)
    blocks = SEQUENCE_TOKENS // BLOCK
    rate_low = 0.25
    rate_high = 1.0
    rates = jnp.exp(jax.random.uniform(rate_key, (blocks, 2 * MEMORY_HEADS), jnp.float32, math.log(rate_low), math.log(rate_high)))
    stable_level = jnp.repeat(rates, BLOCK, axis=0) / SEQUENCE_TOKENS
    slot_places = jax.random.randint(place_key, (3, 2 * MEMORY_HEADS), 0, SEQUENCE_TOKENS)
    loss_values = jax.random.uniform(loss_key, (3, 2 * MEMORY_HEADS), jnp.float32, 0.22, 0.41)
    token_positions = jnp.arange(SEQUENCE_TOKENS, dtype=jnp.int32)[:, None]
    spike_values = jnp.zeros((SEQUENCE_TOKENS, 2 * MEMORY_HEADS), jnp.float32)
    for spike_value in range(3):
        spike_values = spike_values + jnp.where(token_positions == slot_places[spike_value][None, :], loss_values[spike_value][None, :], 0.0)
    return -(stable_level + spike_values)


def level_of(key, extent, cuts, smallest, high):
    gain = 1.0
    for axis_at, blocks in cuts:
        steps = jax.random.uniform(jax.random.fold_in(jax.random.fold_in(key, 6), axis_at), (blocks,), jnp.float32, smallest / len(cuts), high / len(cuts))
        gain = gain * jnp.repeat(jnp.exp(steps), extent[axis_at] // blocks).reshape((-1,) + (1,) * (len(extent) - 1 - axis_at))
    return gain


def gaussian(key, extent, spread, most, cuts=(), kind=jnp.bfloat16):
    array = jax.random.normal(key, extent, jnp.float32) * spread
    if len(cuts) > 0:
        array = level_of(key, extent, cuts, -0.22, 0.18) * array
    return jnp.clip(array, min=-most, max=most).astype(kind)


def setup_inputs(seed: int = 0) -> dict:
    seeds = jax.random.split(jax.random.key(seed), 17)
    return {
        "tokens": gaussian(seeds[0], (SEQUENCE_TOKENS, D), 1.0, 6.0, ((0, 16), (1, 2))),
        "norm_gain": jnp.clip(1.0 + 0.18 * jax.random.normal(seeds[1], (D,), jnp.float32), 0.1, 1.9),
        "glu_value": gaussian(seeds[2], (D, CONV), D ** -0.5, 0.125, ((0, 16), (1, 2))),
        "glu_gate": gaussian(seeds[3], (D, CONV), D ** -0.5, 0.125, ((0, 16), (1, 2))),
        "conv_taps": draw_conv_taps(jax.random.fold_in(seeds[16], 71), 0),
        "ln_gain": jnp.clip(1.0 + 0.18 * jax.random.normal(seeds[5], (CONV,), jnp.float32), 0.1, 1.9),
        "ln_bias": gaussian(seeds[6], (CONV,), 0.5, 3.0, ((0, 2),), jnp.float32),
        "query_weight": gaussian(seeds[7], (D, MEM), D ** -0.5, 0.125, ((0, 16), (1, 2))),
        "key_weight": gaussian(seeds[8], (D, MEM), D ** -0.5, 0.125, ((0, 16), (1, 2))),
        "value_weight": gaussian(seeds[9], (D, MEM), D ** -0.5, 0.125, ((0, 16), (1, 2))),
        "gate_weight": gaussian(seeds[10], (D, 4 * MEMORY_HEADS), D ** -0.5, 0.125),
        "gate_bias": draw_gate_bias(jax.random.fold_in(seeds[16], 71), 0),
        "log_decay_extra": draw_log_decay_extra(jax.random.fold_in(seeds[16], 71), 0),
        "mem_gain": jnp.clip(1.0 + 0.18 * jax.random.normal(seeds[13], (MEM,), jnp.float32), 0.1, 1.9),
        "out_conv": gaussian(seeds[14], (CONV, D), CONV ** -0.5, 0.125, ((0, 2),)),
        "out_mem": gaussian(seeds[15], (MEM, D), MEM ** -0.5, 0.125, ((0, 2),)),
    }


EPS = 1e-06
LOW_START = -1e+30
PRECISE = lax.Precision.HIGHEST

def block_step(carried_state, block_data):
    state_mat, state_vec, stabilizer = carried_state
    queries, key_rows, value_rows, input_gate, log_forget = block_data
    key_scale = HEAD ** (-0.5)
    length = log_forget.shape[-1]
    causal = jnp.tril(jnp.ones((length, length), dtype=bool))
    decay_sum = jnp.cumsum(log_forget, axis=-1)
    log_weight = jnp.where(causal, decay_sum[:, :, None] - decay_sum[:, None, :] + input_gate[:, None, :], -jnp.inf)
    carried = decay_sum + stabilizer[:, None]
    running = jnp.maximum(carried, lax.optimization_barrier(jnp.max(log_weight, axis=-1)))
    inner_weight = jnp.exp(log_weight - running[:, :, None])
    carry_weight = jnp.exp(carried - running)
    raw_scores = jnp.einsum('htd,hsd->hts', queries, key_rows, preferred_element_type=jnp.float32)
    scores = raw_scores * key_scale * inner_weight
    query_wide = queries.astype(jnp.float32)
    numerator = carry_weight[:, :, None] * jnp.einsum('htd,hde->hte', query_wide, state_mat, precision=PRECISE)
    numerator = numerator + jnp.einsum('hts,hse->hte', scores.astype(jnp.bfloat16), value_rows, preferred_element_type=jnp.float32)
    denominator = carry_weight * jnp.einsum('htd,hd->ht', query_wide, state_vec, precision=PRECISE) + lax.optimization_barrier(jnp.sum(scores, axis=-1))
    to_end = decay_sum[:, -1:] - decay_sum + input_gate
    carried_end = decay_sum[:, -1] + stabilizer
    new_stabilizer = jnp.maximum(carried_end, lax.optimization_barrier(jnp.max(to_end, axis=-1)))
    end_weight = jnp.exp(to_end - new_stabilizer[:, None]) * key_scale
    keep_weight = jnp.exp(carried_end - new_stabilizer)
    weighted = key_rows.astype(jnp.float32) * end_weight[:, :, None]
    new_mat = keep_weight[:, None, None] * state_mat + jnp.einsum('hsd,hse->hde', weighted.astype(jnp.bfloat16), value_rows, preferred_element_type=jnp.float32)
    new_vec = keep_weight[:, None] * state_vec + lax.optimization_barrier(jnp.sum(weighted, axis=1))
    return ((new_mat, new_vec, new_stabilizer), (numerator, denominator, running, decay_sum))

def one_direction(queries, key_proj, value_proj, input_gate, log_forget):
    count = SEQUENCE_TOKENS // BLOCK

    def heads_first(tensor):
        return jnp.transpose(tensor.reshape(BLOCK, MEMORY_HEADS, HEAD), (1, 0, 2))

    def step(carried_state, block_data):
        query_blk, key_blk, value_blk, input_blk, forget_blk = block_data
        new_state, results = block_step(carried_state, (heads_first(query_blk), heads_first(key_blk), heads_first(value_blk), input_blk.T, forget_blk.T))
        numerator, denominator, running, _ = results
        return (new_state, numerator / jnp.maximum(jnp.abs(denominator), jnp.exp(-running))[:, :, None])
    start = (jnp.zeros((MEMORY_HEADS, HEAD, HEAD), jnp.float32), jnp.zeros((MEMORY_HEADS, HEAD), jnp.float32), jnp.full((MEMORY_HEADS,), LOW_START, jnp.float32))
    inputs = (queries.reshape(count, BLOCK, MEM), key_proj.reshape(count, BLOCK, MEM), value_proj.reshape(count, BLOCK, MEM), input_gate.reshape(count, BLOCK, MEMORY_HEADS), log_forget.reshape(count, BLOCK, MEMORY_HEADS))
    _, outputs = lax.scan(step, start, inputs)
    return jnp.transpose(outputs, (0, 2, 1, 3)).reshape(SEQUENCE_TOKENS, MEMORY_HEADS, HEAD)

def reference(tokens, norm_gain, glu_value, glu_gate, conv_taps, ln_gain, ln_bias, query_weight, key_weight, value_weight, gate_weight, gate_bias, log_decay_extra, mem_gain, out_conv, out_mem):
    wide = tokens.astype(jnp.float32)
    normed = (wide * lax.rsqrt(lax.optimization_barrier(jnp.mean(wide * wide, axis=-1, keepdims=True)) + EPS) * norm_gain).astype(jnp.bfloat16)
    value_sum = jnp.dot(normed, glu_value, preferred_element_type=jnp.float32)
    gate_sum = jnp.dot(normed, glu_gate, preferred_element_type=jnp.float32)
    glu = (value_sum * jax.nn.sigmoid(gate_sum)).astype(jnp.bfloat16)
    reach = KW // 2
    padded = jnp.pad(glu.astype(jnp.float32), ((reach, reach), (0, 0)))
    conv = jnp.zeros((SEQUENCE_TOKENS, CONV), jnp.float32)
    for offset in range(KW):
        conv = conv + conv_taps[offset] * padded[offset:offset + SEQUENCE_TOKENS]
    chan_mean = lax.optimization_barrier(jnp.mean(conv, axis=-1, keepdims=True))
    chan_var = lax.optimization_barrier(jnp.mean(conv * conv, axis=-1, keepdims=True)) - chan_mean * chan_mean
    normal = (conv - chan_mean) * lax.rsqrt(chan_var + EPS) * ln_gain + ln_bias
    act = (normal * jax.nn.sigmoid(normal)).astype(jnp.bfloat16)
    queries = jnp.dot(normed, query_weight, preferred_element_type=jnp.float32).astype(jnp.bfloat16)
    key_proj = jnp.dot(normed, key_weight, preferred_element_type=jnp.float32).astype(jnp.bfloat16)
    value_proj = jnp.dot(normed, value_weight, preferred_element_type=jnp.float32).astype(jnp.bfloat16)
    gates = (jnp.dot(normed, gate_weight, preferred_element_type=jnp.float32) + gate_bias).reshape(SEQUENCE_TOKENS, 4, MEMORY_HEADS)
    extra = log_decay_extra.reshape(SEQUENCE_TOKENS, 2, MEMORY_HEADS)
    forget_fwd = jax.nn.log_sigmoid(gates[:, 1]) + extra[:, 0]
    forget_bwd = jax.nn.log_sigmoid(gates[:, 3]) + extra[:, 1]
    forward_out = one_direction(queries, key_proj, value_proj, gates[:, 0], forget_fwd)
    backward_out = jnp.flip(one_direction(jnp.flip(queries, 0), jnp.flip(key_proj, 0), jnp.flip(value_proj, 0), jnp.flip(gates[:, 2], 0), jnp.flip(forget_bwd, 0)), 0)
    summed = forward_out + backward_out
    head_norm = summed * lax.rsqrt(lax.optimization_barrier(jnp.mean(summed * summed, axis=-1, keepdims=True)) + EPS)
    memory = (head_norm * mem_gain.reshape(MEMORY_HEADS, HEAD)).reshape(SEQUENCE_TOKENS, MEM).astype(jnp.bfloat16)
    conv_group = CONV // N_TP
    mem_group = MEM // N_TP
    total = jnp.zeros((SEQUENCE_TOKENS, D), jnp.float32)
    for channel_group in range(N_TP):
        conv_cols = act[:, channel_group * conv_group:(channel_group + 1) * conv_group]
        mem_cols = memory[:, channel_group * mem_group:(channel_group + 1) * mem_group]
        partial_sum = jnp.dot(conv_cols, out_conv[channel_group * conv_group:(channel_group + 1) * conv_group], preferred_element_type=jnp.float32)
        partial_sum = partial_sum + jnp.dot(mem_cols, out_mem[channel_group * mem_group:(channel_group + 1) * mem_group], preferred_element_type=jnp.float32)
        total = total + lax.optimization_barrier(partial_sum.astype(jnp.bfloat16)).astype(jnp.float32)
    return total.astype(jnp.bfloat16)
```

```python
import math

import jax
import jax.numpy as jnp
from jax import lax
from jax.sharding import Mesh, PartitionSpec as P

MEMORY_HEADS = 8
HEAD = 256
KW = 31

EPS = 1e-06
PRECISE = lax.Precision.HIGHEST


def parts_of(x):
    first = lax.reduce_precision(x, 8, 7)
    rest = x - first
    second = lax.reduce_precision(rest, 8, 7)
    third = rest - second
    return [p.astype(jnp.bfloat16) for p in (first, second, third)]


def whole_of(a, b, c):
    return a.astype(jnp.float32) + b.astype(jnp.float32) + c.astype(jnp.float32)


def gather_inputs(tokens, weights, extra, inner):
    rows, half = tokens.shape
    gathered = lax.all_gather(tokens, ("inner", "tp"), axis=0)
    tp = gathered.shape[0] // inner
    whole = jnp.transpose(gathered.reshape(inner, tp, rows, half), (0, 2, 1, 3))
    whole = whole.reshape(inner * rows, tp * half)
    depth, columns = weights[0].shape
    width = columns // inner
    packed = jnp.stack([w.reshape(depth, inner, width) for w in weights], axis=2)
    packed = jnp.transpose(packed, (1, 0, 2, 3)).reshape(inner, depth, len(weights) * width)
    if inner > 1:
        packed = lax.all_to_all(packed, "inner", split_axis=0, concat_axis=0, tiled=True)
    pieces = lax.all_gather(packed.reshape(inner * depth, -1), "outer", axis=0, tiled=True)
    extras = lax.all_gather(extra, "inner", axis=0, tiled=True) if inner > 1 else extra
    return whole, pieces, extras


def local_state(keys, values, shifted, level, total, scale):
    weight = jnp.exp(shifted - level[:, None]) * scale
    weighted = keys.astype(jnp.float32) * weight[:, :, None]
    mat = jnp.einsum(
        "hsd,hse->hde", weighted.astype(jnp.bfloat16), values, preferred_element_type=jnp.float32
    )
    return mat, jnp.sum(weighted, axis=1), level + total, total


def packed_state(mat, vec, level, decay):
    spread = lambda x: jnp.broadcast_to(x[:, None], vec.shape)
    rows = parts_of(vec) + parts_of(spread(level)) + parts_of(spread(decay))
    pad = [jnp.zeros_like(rows[0])] * 7
    return jnp.concatenate([mat.astype(jnp.bfloat16), jnp.stack(rows + pad, axis=1)], axis=1)


def incoming(states, reverse):
    count = states.shape[0]
    mats = states[:, :, :HEAD]
    rows = states[:, :, HEAD:]
    vecs = whole_of(rows[:, :, 0], rows[:, :, 1], rows[:, :, 2])
    levels = whole_of(rows[:, :, 3, 0], rows[:, :, 4, 0], rows[:, :, 5, 0])
    decays = whole_of(rows[:, :, 6, 0], rows[:, :, 7, 0], rows[:, :, 8, 0])
    place = lax.axis_index("outer")
    order = jnp.arange(count)
    if reverse:
        ahead = (order > place)[:, None]
        between = (order[None, :] < order[:, None]) & (order[None, :] > place)
    else:
        ahead = (order < place)[:, None]
        between = (order[None, :] > order[:, None]) & (order[None, :] < place)
    lost = jnp.sum(jnp.where(between[:, :, None], decays[None], 0.0), axis=1)
    reach = jnp.where(ahead, levels + lost, -1e30)
    level = jnp.max(reach, axis=0)
    share = jnp.where(ahead, jnp.exp(reach - level[None]), 0.0)
    mat = jnp.sum(share[:, :, None, None] * mats.astype(jnp.float32), axis=0)
    vec = jnp.sum(share[:, :, None] * vecs, axis=0)
    return mat, vec, level


def finish(query_wide, num, den, running, decay, state):
    mat, vec, level = state
    top = jnp.maximum(running, level[:, None])
    local_weight = jnp.exp(running - top)
    carry_weight = jnp.exp(level[:, None] - top)
    num = local_weight[:, :, None] * num + carry_weight[:, :, None] * jnp.einsum(
        "htd,hde->hte", query_wide, mat, precision=PRECISE
    )
    den = local_weight * den + carry_weight * jnp.einsum(
        "htd,hd->ht", query_wide, vec, precision=PRECISE
    )
    return num / jnp.maximum(jnp.abs(den), jnp.exp(-top - decay))[:, :, None]


def make_shards(inner, outer, tp):
    def own(array, dim):
        size = array.shape[dim] // inner
        return lax.dynamic_slice_in_dim(array, lax.axis_index("inner") * size, size, dim)

    def shards(
        tokens,
        norm_gain,
        glu_value,
        glu_gate,
        conv_taps,
        ln_gain,
        ln_bias,
        query_weight,
        key_weight,
        value_weight,
        gate_weight,
        gate_bias,
        log_decay_extra,
        mem_gain,
        out_conv,
        out_mem,
    ):
        taps, gain, bias, mgain = own(conv_taps, 1), own(ln_gain, 0), own(ln_bias, 0), own(mem_gain, 0)
        channels = conv_taps.shape[1] * tp
        width = gain.shape[0]
        heads = mgain.shape[0] // HEAD
        first = (lax.axis_index("tp") * inner + lax.axis_index("inner")) * heads
        whole, weights, extras = gather_inputs(
            tokens, (query_weight, key_weight, value_weight, glu_value, glu_gate),
            log_decay_extra, inner,
        )
        rows = whole.shape[0]
        wide = whole.astype(jnp.float32)
        normed = (
            wide * lax.rsqrt(jnp.mean(wide * wide, axis=-1, keepdims=True) + EPS) * norm_gain
        ).astype(jnp.bfloat16)
        own_gate = lax.dynamic_slice_in_dim(
            gate_weight.reshape(-1, 4, MEMORY_HEADS), first, heads, 2
        )
        own_bias = lax.dynamic_slice_in_dim(gate_bias.reshape(4, MEMORY_HEADS), first, heads, 1)
        gates = lax.dot_general(
            own_gate.reshape(-1, 4 * heads), normed, (((0,), (1,)), ((), ())),
            preferred_element_type=jnp.float32,
        ).reshape(4, heads, rows) + own_bias[:, :, None]
        own_extra = lax.dynamic_slice_in_dim(
            extras.reshape(rows, 2, MEMORY_HEADS), first, heads, 2
        ).transpose(1, 2, 0)
        lf = jax.nn.log_sigmoid(gates[1::2]) + own_extra
        decay_f = jnp.cumsum(lf[0], axis=-1)
        decay_b = lax.cumsum(lf[1], axis=1, reverse=True)
        shifted_f = gates[0] - decay_f
        shifted_b = gates[2] - decay_b
        running_f = lax.cummax(shifted_f, axis=1)
        running_b = lax.cummax(shifted_b, axis=1, reverse=True)

        def project(i):
            return jnp.dot(
                normed, weights[:, i * width : (i + 1) * width],
                preferred_element_type=jnp.float32,
            )

        def heads_first(x):
            return jnp.transpose(x.reshape(rows, heads, HEAD), (1, 0, 2)).astype(jnp.bfloat16)

        keys = heads_first(project(1))
        values = heads_first(project(2))
        scale = HEAD ** (-0.5)
        state_f = local_state(
            keys, values, shifted_f, running_f[:, -1], decay_f[:, -1], scale
        )
        state_b = local_state(keys, values, shifted_b, running_b[:, 0], decay_b[:, 0], scale)
        sent = jnp.stack([packed_state(*state_f), packed_state(*state_b)])
        states = lax.all_gather(sent, "outer", axis=0)

        glu = (project(3) * jax.nn.sigmoid(project(4))).astype(jnp.bfloat16)
        reach = KW // 2
        before = lax.ppermute(glu[rows - reach :], "outer", [(i, i + 1) for i in range(outer - 1)])
        after = lax.ppermute(glu[:reach], "outer", [(i + 1, i) for i in range(outer - 1)])
        queries = heads_first(project(0))

        scores = jnp.einsum("htd,hsd->hts", queries, keys, preferred_element_type=jnp.float32) * scale
        at = jnp.arange(rows)
        causal = at[:, None] >= at[None, :]
        anti = at[:, None] <= at[None, :]

        def local_out(shifted, running, mask):
            weight = jnp.where(
                mask, jnp.exp(jnp.minimum(shifted[:, None, :] - running[:, :, None], 0.0)), 0.0
            )
            part = scores * weight
            num = jnp.einsum(
                "hts,hse->hte", part.astype(jnp.bfloat16), values,
                preferred_element_type=jnp.float32,
            )
            return num, jnp.sum(part, axis=-1)

        num_f, den_f = local_out(shifted_f, running_f, causal)
        num_b, den_b = local_out(shifted_b, running_b, anti)

        padded = jnp.concatenate([before, glu, after], axis=0).astype(jnp.float32)
        conv = jnp.zeros(glu.shape, jnp.float32)
        for offset in range(KW):
            conv = conv + taps[offset] * padded[offset : offset + rows]
        sums = jnp.stack([jnp.sum(conv, axis=-1), jnp.sum(conv * conv, axis=-1)])
        sums = lax.psum(sums, ("inner", "tp")) / channels
        chan_mean = sums[0]
        chan_var = sums[1] - chan_mean * chan_mean
        normal = (conv - chan_mean[:, None]) * lax.rsqrt(chan_var + EPS)[:, None] * gain + bias
        act = (normal * jax.nn.sigmoid(normal)).astype(jnp.bfloat16)

        query_wide = queries.astype(jnp.float32)
        forward = finish(query_wide, num_f, den_f, running_f, decay_f, incoming(states[:, 0], False))
        backward = finish(query_wide, num_b, den_b, running_b, decay_b, incoming(states[:, 1], True))
        summed = forward + backward
        head_norm = summed * lax.rsqrt(jnp.mean(summed * summed, axis=-1, keepdims=True) + EPS)
        head_norm = head_norm * mgain.reshape(heads, HEAD)[:, None, :]
        memory = jnp.transpose(head_norm, (1, 0, 2)).reshape(rows, heads * HEAD).astype(jnp.bfloat16)

        def back(x):
            if inner == 1:
                return x
            return lax.all_to_all(x, "inner", split_axis=0, concat_axis=1, tiled=True)

        result = jnp.dot(back(act), out_conv, preferred_element_type=jnp.float32)
        result = result + jnp.dot(back(memory), out_mem, preferred_element_type=jnp.float32)
        return lax.psum_scatter(
            result.astype(jnp.bfloat16), "tp", scatter_dimension=0, tiled=True
        )

    return shards


def solution(mesh):
    sp, tp = mesh.shape["sp"], mesh.shape["tp"]
    inner = math.gcd(sp, max(MEMORY_HEADS // tp, 1))
    outer = sp // inner
    fine = Mesh(mesh.devices.reshape(outer, inner, tp), ("outer", "inner", "tp"))
    rows = ("outer", "inner")
    in_specs = (
        P(rows, "tp"),
        P(),
        P(rows, "tp"),
        P(rows, "tp"),
        P(None, "tp"),
        P("tp"),
        P("tp"),
        P(rows, "tp"),
        P(rows, "tp"),
        P(rows, "tp"),
        P(),
        P(),
        P(rows, None),
        P("tp"),
        P("tp", None),
        P("tp", None),
    )
    return jax.shard_map(
        make_shards(inner, outer, tp), mesh=fine, in_specs=in_specs,
        out_specs=P(("outer", "inner", "tp"), None), check_vma=False,
    )
```

```python
import functools
import math

import jax
import jax.numpy as jnp
from jax import lax
from jax.experimental import pallas as pl
from jax.experimental.pallas import tpu as pltpu
from jax.sharding import Mesh, PartitionSpec as P

MEMORY_HEADS = 8
HEAD = 256
KW = 31

EPS = 1e-06
PRECISE = lax.Precision.HIGHEST


def parts_of(x):
    first = lax.reduce_precision(x, 8, 7)
    rest = x - first
    second = lax.reduce_precision(rest, 8, 7)
    third = rest - second
    return [p.astype(jnp.bfloat16) for p in (first, second, third)]


def whole_of(a, b, c):
    return a.astype(jnp.float32) + b.astype(jnp.float32) + c.astype(jnp.float32)


MESH = pl.DeviceIdType.MESH


def exchange_kernel(outer, inner, tp, count, *refs):
    tokens, extra = refs[:2]
    weights = refs[2 : 2 + count]
    whole, extras, pieces, stage_w, stage_t, stage_e = refs[2 + count : 8 + count]
    local, a2a_s, a2a_r, tok_s, tok_r, ext_s, ext_r, half_s, half_r, ring_s, ring_r = refs[8 + count :]
    o, i, t = lax.axis_index("outer"), lax.axis_index("inner"), lax.axis_index("tp")
    right, left = lax.rem(o + 1, outer), lax.rem(o + outer - 1, outer)
    rows, half = tokens.shape
    depth = weights[0].shape[0]
    width = pieces.shape[2]

    barrier = pltpu.get_barrier_semaphore()
    greeted = [(o, lax.rem(i + k, inner), t) for k in range(1, inner)]
    greeted += [(o, i, lax.rem(t + k, tp)) for k in range(1, tp)]
    greeted += [(right, i, t), (left, i, t)]
    for device in greeted:
        pl.semaphore_signal(barrier, inc=1, device_id=device, device_id_type=MESH)
    pl.semaphore_wait(barrier, len(greeted))

    def columns(index):
        return pl.ds(pl.multiple_of(index * width, width), width)

    def piece(owner, index):
        start = pl.multiple_of((owner * inner + index) * depth, depth)
        return pieces.at[:, pl.ds(start, depth), :]

    def block(index, core):
        return whole.at[
            pl.ds(pl.multiple_of(index * rows, rows), rows),
            pl.ds(pl.multiple_of(core * half, half), half),
        ]

    def remote(src, dst, send, recv, device):
        return pltpu.make_async_remote_copy(
            src_ref=src, dst_ref=dst, send_sem=send, recv_sem=recv,
            device_id=device, device_id_type=MESH,
        )

    sends = []

    def start(copy):
        copy.start()
        sends.append(copy)

    staged = [
        pltpu.make_async_copy(weights[j].at[:, columns(i)], stage_w.at[j], local.at[j])
        for j in range(count)
    ]
    staged.append(pltpu.make_async_copy(tokens, stage_t, local.at[count]))
    staged.append(pltpu.make_async_copy(extra, stage_e, local.at[count + 1]))
    for copy in staged:
        copy.start()

    def a2a(k, j):
        peer = lax.rem(i + k, inner)
        start_row = pl.multiple_of((o * inner + i) * depth, depth)
        return remote(
            weights[j].at[:, columns(peer)], pieces.at[j, pl.ds(start_row, depth), :],
            a2a_s.at[k - 1, j], a2a_r.at[k - 1, j], (o, peer, t),
        )

    def ring(way, distance, k, src=None):
        index = lax.rem(i + inner - k, inner)
        back = outer - (distance - 1) if way == 0 else distance - 1
        owner = lax.rem(o + back, outer)
        target = right if way == 0 else left
        return remote(
            piece(owner, index) if src is None else src, piece(owner, index),
            ring_s.at[way, distance - 1, k], ring_r.at[way, distance - 1, k], (target, i, t),
        )

    far = outer // 2

    def uses(way, distance, k):
        if 2 * distance < outer:
            return True
        return (k < inner // 2) == (way == 0)

    def tok(k):
        peer = lax.rem(i + k, inner)
        return remote(tokens, block(i, t), tok_s.at[k - 1], tok_r.at[k - 1], (o, peer, t))

    def ext(k):
        peer = lax.rem(i + k, inner)
        return remote(extra, extras.at[i], ext_s.at[k - 1], ext_r.at[k - 1], (o, peer, t))

    def hand(k, c, src=None):
        index = lax.rem(i + inner - k, inner)
        other = lax.rem(t + c, tp)
        return remote(
            block(index, t) if src is None else src, block(index, t),
            half_s.at[k, c - 1], half_r.at[k, c - 1], (o, i, other),
        )

    for k in range(1, inner):
        for j in range(count):
            start(a2a(k, j))
        start(ext(k))
    for j in range(count):
        staged[j].wait()
    for way in range(2):
        start(ring(way, 1, 0, stage_w))
    for k in range(1, inner):
        start(tok(k))
    for c in range(1, tp):
        start(hand(0, c, tokens))
    staged[count].wait()
    staged[count + 1].wait()
    start_own = [
        pltpu.make_async_copy(stage_w, piece(o, i), local.at[0]),
        pltpu.make_async_copy(stage_t, block(i, t), local.at[1]),
        pltpu.make_async_copy(stage_e, extras.at[i], local.at[2]),
    ]
    for copy in start_own:
        copy.start()

    def relay(distance, k):
        for way in range(2):
            if uses(way, distance, k):
                ring(way, distance, k).wait_recv()
                if distance < far and uses(way, distance + 1, k):
                    start(ring(way, distance + 1, k))

    for k in range(1, inner):
        for j in range(count):
            a2a(k, j).wait_recv()
        for way in range(2):
            start(ring(way, 1, k))
        relay(1, k - 1)
    relay(1, inner - 1)
    for k in range(1, inner):
        tok(k).wait_recv()
        for c in range(1, tp):
            start(hand(k, c))
    for distance in range(2, far + 1):
        for k in range(inner):
            relay(distance, k)
    for k in range(1, inner):
        ext(k).wait_recv()
    for k in range(inner):
        for c in range(1, tp):
            hand(k, c).wait_recv()
    for copy in start_own:
        copy.wait()
    for copy in sends:
        copy.wait_send()


def exchange(tokens, weights, extra, outer, inner, tp):
    rows, half = tokens.shape
    depth, columns = weights[0].shape
    width = columns // inner
    count = len(weights)
    turned = extra.T
    dma = pltpu.SemaphoreType.DMA
    far = outer // 2
    any_space = pl.BlockSpec(memory_space=pl.ANY)
    whole, extras, pieces = pl.pallas_call(
        functools.partial(exchange_kernel, outer, inner, tp, count),
        out_shape=(
            jax.ShapeDtypeStruct((inner * rows, tp * half), tokens.dtype),
            jax.ShapeDtypeStruct((inner,) + turned.shape, turned.dtype),
            jax.ShapeDtypeStruct((count, outer * inner * depth, width), weights[0].dtype),
        ),
        in_specs=[any_space] * (2 + count),
        out_specs=(any_space,) * 3,
        scratch_shapes=[
            pltpu.VMEM((count, depth, width), weights[0].dtype),
            pltpu.VMEM((rows, half), tokens.dtype),
            pltpu.VMEM(turned.shape, turned.dtype),
            dma((count + 2,)),
            dma((inner - 1, count)), dma((inner - 1, count)),
            dma((inner - 1,)), dma((inner - 1,)),
            dma((inner - 1,)), dma((inner - 1,)),
            dma((inner, tp - 1)), dma((inner, tp - 1)),
            dma((2, far, inner)), dma((2, far, inner)),
        ],
        compiler_params=pltpu.CompilerParams(collective_id=0, has_side_effects=True),
    )(tokens, turned, *weights)
    extras = jnp.transpose(extras, (1, 0, 2)).reshape(turned.shape[0], inner * rows)
    return whole, pieces, extras


def gather_inputs(tokens, weights, extra, inner):
    rows, half = tokens.shape
    gathered = lax.all_gather(tokens, ("inner", "tp"), axis=0)
    tp = gathered.shape[0] // inner
    whole = jnp.transpose(gathered.reshape(inner, tp, rows, half), (0, 2, 1, 3))
    whole = whole.reshape(inner * rows, tp * half)
    depth, columns = weights[0].shape
    width = columns // inner
    packed = jnp.stack([w.reshape(depth, inner, width) for w in weights], axis=2)
    packed = jnp.transpose(packed, (1, 0, 2, 3)).reshape(inner, depth, len(weights) * width)
    if inner > 1:
        packed = lax.all_to_all(packed, "inner", split_axis=0, concat_axis=0, tiled=True)
    pieces = lax.all_gather(packed.reshape(inner * depth, -1), "outer", axis=0, tiled=True)
    pieces = pieces.reshape(-1, len(weights), width).transpose(1, 0, 2)
    extras = lax.all_gather(extra, "inner", axis=0, tiled=True) if inner > 1 else extra
    return whole, pieces, extras.T


def local_state(keys, values, shifted, level, total, scale):
    weight = jnp.exp(shifted - level[:, None]) * scale
    weighted = keys.astype(jnp.float32) * weight[:, :, None]
    mat = jnp.einsum(
        "hsd,hse->hde", weighted.astype(jnp.bfloat16), values, preferred_element_type=jnp.float32
    )
    return mat, jnp.sum(weighted, axis=1), level + total, total


def packed_state(mat, vec, level, decay):
    spread = lambda x: jnp.broadcast_to(x[:, None], vec.shape)
    rows = parts_of(vec) + parts_of(spread(level)) + parts_of(spread(decay))
    pad = [jnp.zeros_like(rows[0])] * 7
    return jnp.concatenate([mat.astype(jnp.bfloat16), jnp.stack(rows + pad, axis=1)], axis=1)


def incoming(states, reverse):
    count = states.shape[0]
    mats = states[:, :, :HEAD]
    rows = states[:, :, HEAD:]
    vecs = whole_of(rows[:, :, 0], rows[:, :, 1], rows[:, :, 2])
    levels = whole_of(rows[:, :, 3, 0], rows[:, :, 4, 0], rows[:, :, 5, 0])
    decays = whole_of(rows[:, :, 6, 0], rows[:, :, 7, 0], rows[:, :, 8, 0])
    place = lax.axis_index("outer")
    order = jnp.arange(count)
    if reverse:
        ahead = (order > place)[:, None]
        between = (order[None, :] < order[:, None]) & (order[None, :] > place)
    else:
        ahead = (order < place)[:, None]
        between = (order[None, :] > order[:, None]) & (order[None, :] < place)
    lost = jnp.sum(jnp.where(between[:, :, None], decays[None], 0.0), axis=1)
    reach = jnp.where(ahead, levels + lost, -1e30)
    level = jnp.max(reach, axis=0)
    share = jnp.where(ahead, jnp.exp(reach - level[None]), 0.0)
    mat = jnp.sum(share[:, :, None, None] * mats.astype(jnp.float32), axis=0)
    vec = jnp.sum(share[:, :, None] * vecs, axis=0)
    return mat, vec, level


def finish(query_wide, num, den, running, decay, state):
    mat, vec, level = state
    top = jnp.maximum(running, level[:, None])
    local_weight = jnp.exp(running - top)
    carry_weight = jnp.exp(level[:, None] - top)
    num = local_weight[:, :, None] * num + carry_weight[:, :, None] * jnp.einsum(
        "htd,hde->hte", query_wide, mat, precision=PRECISE
    )
    den = local_weight * den + carry_weight * jnp.einsum(
        "htd,hd->ht", query_wide, vec, precision=PRECISE
    )
    return num / jnp.maximum(jnp.abs(den), jnp.exp(-top - decay))[:, :, None]


def make_shards(inner, outer, tp):
    def own(array, dim):
        size = array.shape[dim] // inner
        return lax.dynamic_slice_in_dim(array, lax.axis_index("inner") * size, size, dim)

    def shards(
        tokens,
        norm_gain,
        glu_value,
        glu_gate,
        conv_taps,
        ln_gain,
        ln_bias,
        query_weight,
        key_weight,
        value_weight,
        gate_weight,
        gate_bias,
        log_decay_extra,
        mem_gain,
        out_conv,
        out_mem,
    ):
        taps, gain, bias, mgain = own(conv_taps, 1), own(ln_gain, 0), own(ln_bias, 0), own(mem_gain, 0)
        channels = conv_taps.shape[1] * tp
        width = gain.shape[0]
        heads = mgain.shape[0] // HEAD
        first = (lax.axis_index("tp") * inner + lax.axis_index("inner")) * heads
        stacked = (query_weight, key_weight, value_weight, glu_value, glu_gate)
        if inner > 1 and tp > 1 and outer > 2:
            whole, weights, extras = exchange(tokens, stacked, log_decay_extra, outer, inner, tp)
        else:
            whole, weights, extras = gather_inputs(tokens, stacked, log_decay_extra, inner)
        rows = whole.shape[0]
        wide = whole.astype(jnp.float32)
        normed = (
            wide * lax.rsqrt(jnp.mean(wide * wide, axis=-1, keepdims=True) + EPS) * norm_gain
        ).astype(jnp.bfloat16)
        own_gate = lax.dynamic_slice_in_dim(
            gate_weight.reshape(-1, 4, MEMORY_HEADS), first, heads, 2
        )
        own_bias = lax.dynamic_slice_in_dim(gate_bias.reshape(4, MEMORY_HEADS), first, heads, 1)
        gates = lax.dot_general(
            own_gate.reshape(-1, 4 * heads), normed, (((0,), (1,)), ((), ())),
            preferred_element_type=jnp.float32,
        ).reshape(4, heads, rows) + own_bias[:, :, None]
        own_extra = lax.dynamic_slice_in_dim(
            extras.reshape(2, MEMORY_HEADS, rows), first, heads, 1
        )
        lf = jax.nn.log_sigmoid(gates[1::2]) + own_extra
        decay_f = jnp.cumsum(lf[0], axis=-1)
        decay_b = lax.cumsum(lf[1], axis=1, reverse=True)
        shifted_f = gates[0] - decay_f
        shifted_b = gates[2] - decay_b
        running_f = lax.cummax(shifted_f, axis=1)
        running_b = lax.cummax(shifted_b, axis=1, reverse=True)

        def project(i):
            return jnp.dot(normed, weights[i], preferred_element_type=jnp.float32)

        def heads_first(x):
            return jnp.transpose(x.reshape(rows, heads, HEAD), (1, 0, 2)).astype(jnp.bfloat16)

        keys = heads_first(project(1))
        values = heads_first(project(2))
        scale = HEAD ** (-0.5)
        state_f = local_state(
            keys, values, shifted_f, running_f[:, -1], decay_f[:, -1], scale
        )
        state_b = local_state(keys, values, shifted_b, running_b[:, 0], decay_b[:, 0], scale)
        sent = jnp.stack([packed_state(*state_f), packed_state(*state_b)])
        states = lax.all_gather(sent, "outer", axis=0)

        glu = (project(3) * jax.nn.sigmoid(project(4))).astype(jnp.bfloat16)
        reach = KW // 2
        before = lax.ppermute(glu[rows - reach :], "outer", [(i, i + 1) for i in range(outer - 1)])
        after = lax.ppermute(glu[:reach], "outer", [(i + 1, i) for i in range(outer - 1)])
        queries = heads_first(project(0))

        scores = jnp.einsum("htd,hsd->hts", queries, keys, preferred_element_type=jnp.float32) * scale
        at = jnp.arange(rows)
        causal = at[:, None] >= at[None, :]
        anti = at[:, None] <= at[None, :]

        def local_out(shifted, running, mask):
            weight = jnp.where(
                mask, jnp.exp(jnp.minimum(shifted[:, None, :] - running[:, :, None], 0.0)), 0.0
            )
            part = scores * weight
            num = jnp.einsum(
                "hts,hse->hte", part.astype(jnp.bfloat16), values,
                preferred_element_type=jnp.float32,
            )
            return num, jnp.sum(part, axis=-1)

        num_f, den_f = local_out(shifted_f, running_f, causal)
        num_b, den_b = local_out(shifted_b, running_b, anti)

        padded = jnp.concatenate([before, glu, after], axis=0).astype(jnp.float32)
        conv = jnp.zeros(glu.shape, jnp.float32)
        for offset in range(KW):
            conv = conv + taps[offset] * padded[offset : offset + rows]
        sums = jnp.stack([jnp.sum(conv, axis=-1), jnp.sum(conv * conv, axis=-1)])
        sums = lax.psum(sums, ("inner", "tp")) / channels
        chan_mean = sums[0]
        chan_var = sums[1] - chan_mean * chan_mean
        normal = (conv - chan_mean[:, None]) * lax.rsqrt(chan_var + EPS)[:, None] * gain + bias
        act = (normal * jax.nn.sigmoid(normal)).astype(jnp.bfloat16)

        query_wide = queries.astype(jnp.float32)
        forward = finish(query_wide, num_f, den_f, running_f, decay_f, incoming(states[:, 0], False))
        backward = finish(query_wide, num_b, den_b, running_b, decay_b, incoming(states[:, 1], True))
        summed = forward + backward
        head_norm = summed * lax.rsqrt(jnp.mean(summed * summed, axis=-1, keepdims=True) + EPS)
        head_norm = head_norm * mgain.reshape(heads, HEAD)[:, None, :]
        memory = jnp.transpose(head_norm, (1, 0, 2)).reshape(rows, heads * HEAD).astype(jnp.bfloat16)

        def back(x):
            if inner == 1:
                return x
            return lax.all_to_all(x, "inner", split_axis=0, concat_axis=1, tiled=True)

        result = jnp.dot(back(act), out_conv, preferred_element_type=jnp.float32)
        result = result + jnp.dot(back(memory), out_mem, preferred_element_type=jnp.float32)
        return lax.psum_scatter(
            result.astype(jnp.bfloat16), "tp", scatter_dimension=0, tiled=True
        )

    return shards


def solution(mesh):
    sp, tp = mesh.shape["sp"], mesh.shape["tp"]
    inner = math.gcd(sp, max(MEMORY_HEADS // tp, 1))
    outer = sp // inner
    fine = Mesh(mesh.devices.reshape(outer, inner, tp), ("outer", "inner", "tp"))
    rows = ("outer", "inner")
    in_specs = (
        P(rows, "tp"),
        P(),
        P(rows, "tp"),
        P(rows, "tp"),
        P(None, "tp"),
        P("tp"),
        P("tp"),
        P(rows, "tp"),
        P(rows, "tp"),
        P(rows, "tp"),
        P(),
        P(),
        P(rows, None),
        P("tp"),
        P("tp", None),
        P("tp", None),
    )
    return jax.shard_map(
        make_shards(inner, outer, tp), mesh=fine, in_specs=in_specs,
        out_specs=P(("outer", "inner", "tp"), None), check_vma=False,
    )
```
